32 devices in a mesh: grp: 2 (over y), sp: 4 (over z), tp: 4 (over x, core).
Axes of the slice: x: 2, y: 2, z: 4, core: 2. Of those that a mesh axis runs over, the one named last changes fastest.
Arguments:
- tokens_in: bfloat16 [3072, 4096], P(('grp', 'sp')), parts along dimension 0, may hold values from -6 to 6
- norm_gain: float32 [4096], replicated, may hold values from 0.1 to 1.9
- window_query: bfloat16 [4096, 1024], P('sp', 'tp'), may hold values from -0.09375 to 0.09375
- window_key: bfloat16 [4096, 512], P('sp', 'tp'), may hold values from -0.09375 to 0.09375
- window_value: bfloat16 [4096, 512], P('sp', 'tp'), may hold values from -0.09375 to 0.09375
- window_query_gain: float32 [64], replicated, may hold values from 0.6 to 16
- window_key_gain: float32 [64], replicated, may hold values from 0.6 to 16
- sink_logit: float32 [16], P('tp'), may hold values from 1 to 6
- dense_query: bfloat16 [4096, 1024], P('sp', 'tp'), may hold values from -0.09375 to 0.09375
- dense_key: bfloat16 [4096, 512], P('sp', 'tp'), may hold values from -0.09375 to 0.09375
- dense_value: bfloat16 [4096, 512], P('sp', 'tp'), may hold values from -0.09375 to 0.09375
- dense_query_gain: float32 [64], replicated, may hold values from 1 to 14
- dense_key_gain: float32 [64], replicated, may hold values from 1 to 14
- window_out: bfloat16 [1024, 4096], P('tp', 'sp'), may hold values from -1.5 to 1.5
- dense_out: bfloat16 [1024, 4096], P('tp', 'sp'), may hold values from -3 to 3
Outputs:
- mixed_out: bfloat16 [3072, 4096], P(('grp', 'sp', 'tp')), parts along dimension 0
The draws below stay inside these ranges and needn't reach their ends.
There are 2 independent parts, one for each index of `grp`. The reference program is written for one: setup_inputs(seed, part) draws one part's arguments, and reference() takes and returns one part's arrays. A program takes and returns all parts, laid end to end along the dimension named above; an argument that names none is the same for every part. Nothing has to cross between parts.
All inputs are finite; a program needn't handle non-finite values.
Results may differ from the reference program's by a relative error of at most 0.03.
The reference program's roundings to bfloat16 on the way count: a program that leaves them out, or rounds other values in their place, can miss the bound.
Values may be sent and summed in bfloat16 or wider, within the bound.
A program may use at most 64 MiB of HBM per device.

```python
import jax
import jax.numpy as jnp
from jax import lax

D = 4096
B_HEADS = 16
B_KV = 8
C_HEADS = 16
C_KV = 8
HD = 64
WINDOW = 128
GRID_W = 64
TOKENS = 1536
N_TP = 4


def gain_values(key, salt, low, high, hidden_low, hidden_high):
    subkey = jax.random.fold_in(key, salt)
    return jax.random.uniform(subkey, (HD,), jnp.float32, low, high)


def draw_window_query_gain(key, part):
    return gain_values(key, 101, 0.6, 1.6, 12.0, 16.0)


def draw_window_key_gain(key, part):
    return gain_values(key, 102, 0.6, 1.6, 12.0, 16.0)


def draw_dense_query_gain(key, part):
    return gain_values(key, 103, 1.0, 1.8, 10.0, 14.0)


def draw_dense_key_gain(key, part):
    return gain_values(key, 104, 1.0, 1.8, 10.0, 14.0)


def steps_of(key, shape, pieces, least, top_value):
    loudness = 1.0
    for axis_at, blocks in pieces:
        draws = jax.random.uniform(jax.random.fold_in(jax.random.fold_in(key, 6), axis_at), (blocks,), jnp.float32, least / len(pieces), top_value / len(pieces))
        loudness = loudness * jnp.repeat(jnp.exp(draws), shape[axis_at] // blocks).reshape((-1,) + (1,) * (len(shape) - 1 - axis_at))
    return loudness


def noise(key, extent, deviation, reach, cuts=(), held_as=jnp.bfloat16):
    loudness = steps_of(key, extent, cuts, -0.22, 0.18) if cuts else 1.0
    entries = jax.random.normal(key, extent, jnp.float32) * deviation * loudness
    return jnp.minimum(jnp.maximum(entries, -reach), reach).astype(held_as)


def setup_inputs(seed: int = 0, part: int = 0) -> dict:
    seeds = jax.random.split(jax.random.key(seed), 16)
    part_splits = jax.random.split(jax.random.fold_in(seeds[15], part), 16)
    tokens_in = noise(part_splits[0], (TOKENS, D), 1.0, 6.0, ((0, 4),))
    norm_gain = jnp.clip(1.0 + 0.18 * jax.random.normal(seeds[1], (D,), jnp.float32), 0.1, 1.9)
    window_query = noise(seeds[2], (D, B_HEADS * HD), D ** -0.5, 0.09375, ((0, 4), (1, 4)))
    window_key = noise(seeds[3], (D, B_KV * HD), D ** -0.5, 0.09375, ((0, 4), (1, 4)))
    window_value = noise(seeds[4], (D, B_KV * HD), D ** -0.5, 0.09375, ((0, 4), (1, 4)))
    window_query_gain = draw_window_query_gain(jax.random.fold_in(seeds[15], 71), part)
    window_key_gain = draw_window_key_gain(jax.random.fold_in(seeds[15], 71), part)
    sink_logit = jnp.clip(1.0 + 5.0 * jax.random.uniform(seeds[7], (B_HEADS,), jnp.float32) ** steps_of(seeds[7], (B_HEADS,), ((0, 4),), -0.2, 0.2), 1.0, 6.0)
    dense_query = noise(seeds[8], (D, C_HEADS * HD), D ** -0.5, 0.09375, ((0, 4), (1, 4)))
    dense_key = noise(seeds[9], (D, C_KV * HD), D ** -0.5, 0.09375, ((0, 4), (1, 4)))
    dense_value = noise(seeds[10], (D, C_KV * HD), D ** -0.5, 0.09375, ((0, 4), (1, 4)))
    dense_query_gain = draw_dense_query_gain(jax.random.fold_in(seeds[15], 71), part)
    dense_key_gain = draw_dense_key_gain(jax.random.fold_in(seeds[15], 71), part)
    window_out = noise(seeds[13], (B_HEADS * HD, D), 0.25, 1.5, ((0, 4), (1, 4)))
    dense_out = noise(seeds[14], (C_HEADS * HD, D), 0.5, 3.0, ((0, 4), (1, 4)))
    return {"tokens_in": tokens_in, "norm_gain": norm_gain, "window_query": window_query, "window_key": window_key, "window_value": window_value, "window_query_gain": window_query_gain, "window_key_gain": window_key_gain, "sink_logit": sink_logit, "dense_query": dense_query, "dense_key": dense_key, "dense_value": dense_value, "dense_query_gain": dense_query_gain, "dense_key_gain": dense_key_gain, "window_out": window_out, "dense_out": dense_out}


EPS = 1e-06
THETA = 10000.0

def store(values):
    return lax.optimization_barrier(values.astype(jnp.bfloat16))

def rope_table(places, width):
    inverse = THETA ** (-jnp.arange(0, width, 2, dtype=jnp.float32) / width)
    angles = places.astype(jnp.float32)[:, None] * inverse[None, :]
    angles = jnp.concatenate([angles, angles], axis=-1)
    return (jnp.cos(angles), jnp.sin(angles))

def turn(values, tables):
    cosine, sine = tables
    middle = values.shape[-1] // 2
    rotated = jnp.concatenate([-values[..., middle:], values[..., :middle]], axis=-1)
    return values * cosine[:, None, :] + rotated * sine[:, None, :]

def head_norm(projected, gain):
    width = gain.shape[0]
    heads = projected.reshape(projected.shape[0], -1, width)
    return heads * lax.rsqrt(lax.optimization_barrier(jnp.mean(heads * heads, axis=-1, keepdims=True)) + EPS) * gain

def line_heads(projected, gain, places):
    normed = head_norm(projected, gain)
    return turn(normed, rope_table(places, gain.shape[0])).reshape(projected.shape)

def grid_heads(projected, gain, places):
    normed = head_norm(projected, gain)
    middle = gain.shape[0] // 2
    by_row = turn(normed[..., :middle], rope_table(places // GRID_W, middle))
    by_col = turn(normed[..., middle:], rope_table(places % GRID_W, middle))
    return jnp.concatenate([by_row, by_col], axis=-1).reshape(projected.shape)

def banded(query, keys_ext, values_ext, offset, total_len, sink_logit):
    length = query.shape[0]
    kv_heads = keys_ext.shape[1] // HD
    group_size = query.shape[1] // (HD * kv_heads)
    block_count = length // WINDOW
    query_blocks = query.astype(jnp.float32).reshape(block_count, WINDOW, kv_heads, group_size, HD)
    key_blocks = keys_ext.astype(jnp.float32).reshape(block_count + 2, WINDOW, kv_heads, HD)
    value_blocks = values_ext.astype(jnp.float32).reshape(block_count + 2, WINDOW, kv_heads, HD)
    key_near = jnp.concatenate([key_blocks[:-2], key_blocks[1:-1], key_blocks[2:]], axis=1)
    value_near = jnp.concatenate([value_blocks[:-2], value_blocks[1:-1], value_blocks[2:]], axis=1)
    scores = jnp.einsum('nqhgd,nkhd->nhgqk', query_blocks, key_near) * HD ** (-0.5)
    query_pos = offset + jnp.arange(length, dtype=jnp.int32).reshape(block_count, WINDOW)
    key_pos = offset - WINDOW + (jnp.arange(block_count, dtype=jnp.int32)[:, None] * WINDOW + jnp.arange(3 * WINDOW, dtype=jnp.int32)[None, :])
    valid = (jnp.abs(query_pos[:, :, None] - key_pos[:, None, :]) <= WINDOW) & (key_pos >= 0)[:, None, :] & (key_pos < total_len)[:, None, :]
    scores = jnp.where(valid[:, None, None], scores, -jnp.inf)
    floor = sink_logit.reshape(kv_heads, group_size)[None, :, :, None, None]
    top = jnp.maximum(lax.optimization_barrier(jnp.max(scores, axis=-1, keepdims=True)), floor)
    expon = jnp.exp(scores - top)
    weights = store(expon / (lax.optimization_barrier(jnp.sum(expon, axis=-1, keepdims=True)) + jnp.exp(floor - top)))
    result = jnp.einsum('nhgqk,nkhd->nqhgd', weights.astype(jnp.float32), value_near)
    return result.reshape(length, -1)

def dense_attention(query, keys, values):
    length = query.shape[0]
    kv_heads = keys.shape[1] // HD
    group_size = query.shape[1] // (HD * kv_heads)
    if length % 256 == 0:
        block = 256
    elif length % 128 == 0:
        block = 128
    else:
        block = length
    query_blocks = query.astype(jnp.float32).reshape(length // block, block, kv_heads, group_size, HD)
    key_heads = keys.astype(jnp.float32).reshape(length, kv_heads, HD)
    value_heads = values.astype(jnp.float32).reshape(length, kv_heads, HD)

    def one_block(query_block):
        scores = jnp.einsum('qhgd,khd->hgqk', query_block, key_heads) * HD ** (-0.5)
        top = lax.optimization_barrier(jnp.max(scores, axis=-1, keepdims=True))
        expon = jnp.exp(scores - top)
        total = lax.optimization_barrier(jnp.sum(expon, axis=-1))
        rounded = store(expon).astype(jnp.float32)
        summed = jnp.einsum('hgqk,khd->qhgd', rounded, value_heads)
        return summed / jnp.transpose(total, (2, 0, 1))[..., None]
    result = lax.map(one_block, query_blocks)
    return result.reshape(length, -1)

def reference(tokens_in, norm_gain, window_query, window_key, window_value, window_query_gain, window_key_gain, sink_logit, dense_query, dense_key, dense_value, dense_query_gain, dense_key_gain, window_out, dense_out):
    inputs = tokens_in.astype(jnp.float32)
    normed = (inputs * lax.rsqrt(lax.optimization_barrier(jnp.mean(inputs * inputs, axis=-1, keepdims=True)) + EPS) * norm_gain).astype(jnp.bfloat16)

    def project(weight):
        return jnp.dot(normed, weight, preferred_element_type=jnp.float32)
    places = jnp.arange(TOKENS, dtype=jnp.int32)
    query_win = store(line_heads(project(window_query), window_query_gain, places))
    key_win = store(line_heads(project(window_key), window_key_gain, places))
    value_win = store(project(window_value))
    query_den = store(grid_heads(project(dense_query), dense_query_gain, places))
    key_den = store(grid_heads(project(dense_key), dense_key_gain, places))
    value_den = store(project(dense_value))
    margin = ((WINDOW, WINDOW), (0, 0))
    att_win = store(banded(query_win, jnp.pad(key_win, margin), jnp.pad(value_win, margin), 0, TOKENS, sink_logit))
    att_den = store(dense_attention(query_den, key_den, value_den))
    win_parts = att_win.reshape(TOKENS, N_TP, -1).transpose(1, 0, 2)
    den_parts = att_den.reshape(TOKENS, N_TP, -1).transpose(1, 0, 2)
    win_rows = window_out.reshape(N_TP, -1, D)
    den_rows = dense_out.reshape(N_TP, -1, D)

    def add_group(running, members):
        win_part, win_weight, den_part, den_weight = members
        partial_value = jnp.dot(win_part, win_weight, preferred_element_type=jnp.float32) + jnp.dot(den_part, den_weight, preferred_element_type=jnp.float32)
        return (running + store(partial_value).astype(jnp.float32), None)
    running, unused = lax.scan(add_group, jnp.zeros((TOKENS, D), jnp.float32), (win_parts, win_rows, den_parts, den_rows))
    return running.astype(jnp.bfloat16)
```

```python
import jax
import jax.numpy as jnp
from jax import lax
from jax.experimental import pallas as pl
from jax.experimental.pallas import tpu as pltpu
from jax.sharding import PartitionSpec as P

HD = 64
WINDOW = 128
GRID_W = 64


EPS = 1e-06
THETA = 10000.0


def extended(block, sides, width):
    for axis, dim in sides:
        count = lax.axis_size(axis)
        forward = [(i, i + 1) for i in range(count - 1)]
        backward = [(target, source) for source, target in forward]
        low = lax.ppermute(
            lax.slice_in_dim(block, block.shape[dim] - width, None, axis=dim), axis, forward
        )
        high = lax.ppermute(lax.slice_in_dim(block, 0, width, axis=dim), axis, backward)
        block = jnp.concatenate([low, block, high], axis=dim)
    return block


def rope_table(places, width):
    inverse = THETA ** (-jnp.arange(0, width, 2, dtype=jnp.float32) / width)
    angles = places.astype(jnp.float32)[:, None] * inverse[None, :]
    angles = jnp.concatenate([angles, angles], axis=-1)
    return (jnp.cos(angles), jnp.sin(angles))


def turn(values, tables):
    cosine, sine = tables
    middle = values.shape[-1] // 2
    rotated = jnp.concatenate([-values[..., middle:], values[..., :middle]], axis=-1)
    return values * cosine[:, None, :] + rotated * sine[:, None, :]


def head_norm(projected, gain):
    width = gain.shape[0]
    heads = projected.reshape(projected.shape[0], -1, width)
    return heads * lax.rsqrt(jnp.mean(heads * heads, axis=-1, keepdims=True) + EPS) * gain


def line_heads(projected, gain, places):
    normed = head_norm(projected, gain)
    turned = turn(normed, rope_table(places, gain.shape[0]))
    return turned.reshape(projected.shape).astype(jnp.bfloat16)


def grid_heads(projected, gain, places):
    normed = head_norm(projected, gain)
    middle = gain.shape[0] // 2
    by_row = turn(normed[..., :middle], rope_table(places // GRID_W, middle))
    by_col = turn(normed[..., middle:], rope_table(places % GRID_W, middle))
    joined = jnp.concatenate([by_row, by_col], axis=-1)
    return joined.reshape(projected.shape).astype(jnp.bfloat16)


def banded(query, keys_ext, values_ext, offset, total_len, sink_logit):
    length = query.shape[0]
    kv_heads = keys_ext.shape[1] // HD
    group_size = query.shape[1] // (HD * kv_heads)
    block_count = length // WINDOW
    query_blocks = query.reshape(block_count, WINDOW, kv_heads, group_size, HD)
    key_blocks = keys_ext.reshape(block_count + 2, WINDOW, kv_heads, HD)
    value_blocks = values_ext.reshape(block_count + 2, WINDOW, kv_heads, HD)
    key_near = jnp.concatenate([key_blocks[:-2], key_blocks[1:-1], key_blocks[2:]], axis=1)
    value_near = jnp.concatenate([value_blocks[:-2], value_blocks[1:-1], value_blocks[2:]], axis=1)
    scores = jnp.einsum(
        "nqhgd,nkhd->nhgqk", query_blocks, key_near, preferred_element_type=jnp.float32
    ) * HD ** (-0.5)
    query_pos = offset + jnp.arange(length, dtype=jnp.int32).reshape(block_count, WINDOW)
    key_pos = (
        offset
        - WINDOW
        + (
            jnp.arange(block_count, dtype=jnp.int32)[:, None] * WINDOW
            + jnp.arange(3 * WINDOW, dtype=jnp.int32)[None, :]
        )
    )
    valid = (
        (jnp.abs(query_pos[:, :, None] - key_pos[:, None, :]) <= WINDOW)
        & (key_pos >= 0)[:, None, :]
        & (key_pos < total_len)[:, None, :]
    )
    scores = jnp.where(valid[:, None, None], scores, -jnp.inf)
    floor = sink_logit.reshape(kv_heads, group_size)[None, :, :, None, None]
    top = jnp.maximum(jnp.max(scores, axis=-1, keepdims=True), floor)
    expon = jnp.exp(scores - top)
    weights = (expon / (jnp.sum(expon, axis=-1, keepdims=True) + jnp.exp(floor - top))).astype(
        jnp.bfloat16
    )
    result = jnp.einsum(
        "nhgqk,nkhd->nqhgd", weights, value_near, preferred_element_type=jnp.float32
    )
    return result.astype(jnp.bfloat16).reshape(length, -1)


def dense_whole(query, keys, values):
    length = query.shape[0]
    kv_heads = keys.shape[1] // HD
    group_size = query.shape[1] // (HD * kv_heads)
    block = 128
    query_blocks = query.reshape(length // block, block, kv_heads, group_size, HD)
    key_heads = keys.reshape(-1, kv_heads, HD)
    value_heads = values.reshape(-1, kv_heads, HD)

    def one_block(query_block):
        scores = jnp.einsum(
            "qhgd,khd->hgqk", query_block, key_heads, preferred_element_type=jnp.float32
        ) * HD ** (-0.5)
        top = jnp.max(scores, axis=-1, keepdims=True)
        expon = jnp.exp(scores - top)
        total = jnp.sum(expon, axis=-1)
        summed = jnp.einsum(
            "hgqk,khd->qhgd",
            expon.astype(jnp.bfloat16),
            value_heads,
            preferred_element_type=jnp.float32,
        )
        return (summed / jnp.transpose(total, (2, 0, 1))[..., None]).astype(jnp.bfloat16)

    result = lax.map(one_block, query_blocks)
    return result.reshape(length, -1)


MESH = pl.DeviceIdType.MESH
HALVES = 2


class LineGather:
    def __init__(self, own, buf, z_recv, y_recv, r_send, l_send, y_send):
        self.own, self.buf = own, buf
        self.z_recv, self.y_recv = z_recv, y_recv
        self.r_send, self.l_send, self.y_send = r_send, l_send, y_send
        self.n = lax.axis_size("sp")
        self.s = lax.axis_index("sp")
        self.g = lax.axis_index("grp")
        self.chunks = z_recv.shape[1]
        self.half = own.shape[0] // HALVES
        self.size = self.half // self.chunks

    def rows(self, half, c):
        return pl.ds(pl.multiple_of(half * self.half + c * self.size, self.size), self.size)

    def copy(self, src, o, c, sem, recv, target, half):
        return pltpu.make_async_remote_copy(
            src_ref=src,
            dst_ref=self.buf.at[o, self.rows(half, c)],
            send_sem=sem.at[o, c],
            recv_sem=recv.at[o, c],
            device_id=target,
            device_id_type=MESH,
        )

    def right(self, src, o, c):
        return self.copy(src, o, c, self.r_send, self.z_recv, {"sp": lax.rem(self.s + 1, self.n)}, self.g)

    def left(self, src, o, c):
        return self.copy(
            src, o, c, self.l_send, self.z_recv, {"sp": lax.rem(self.s + self.n - 1, self.n)}, self.g
        )

    def twin(self, o, c, half):
        return self.copy(
            self.buf.at[o, self.rows(half, c)], o, c, self.y_send, self.y_recv, {"grp": 1 - self.g}, half
        )

    def start(self):
        for c in range(self.chunks):
            mine = self.own.at[self.rows(self.g, c)]

            @pl.when(self.s + 1 < self.n)
            def _():
                self.right(mine, self.s, c).start()

            @pl.when(self.s > 0)
            def _():
                self.left(mine, self.s, c).start()

    def forward(self, d):
        for c in range(self.chunks):

            @pl.when(self.s - d >= 0)
            def _():
                o = self.s - d
                there = self.buf.at[o, self.rows(self.g, c)]
                self.right(there, o, c).wait_recv()

                @pl.when(self.s + 1 < self.n)
                def _():
                    self.right(there, o, c).start()

                self.twin(o, c, self.g).start()

            @pl.when(self.s + d < self.n)
            def _():
                o = self.s + d
                there = self.buf.at[o, self.rows(self.g, c)]
                self.left(there, o, c).wait_recv()

                @pl.when(self.s > 0)
                def _():
                    self.left(there, o, c).start()

                self.twin(o, c, self.g).start()

    def use(self, d, fn):
        @pl.when(self.s - d >= 0)
        def _():
            for c in range(self.chunks):
                self.twin(self.s - d, c, 1 - self.g).wait_recv()
            fn(self.s - d)

        @pl.when(self.s + d < self.n)
        def _():
            for c in range(self.chunks):
                self.twin(self.s + d, c, 1 - self.g).wait_recv()
            fn(self.s + d)

    def run(self, fn):
        self.forward(1)

        @pl.loop(2, self.n)
        def _(d):
            self.forward(d)
            self.use(d - 1, fn)

        self.use(self.n - 1, fn)

    def finish(self):
        @pl.loop(0, self.n)
        def _(o):
            for c in range(self.chunks):
                there = self.buf.at[o, self.rows(self.g, c)]

                @pl.when((o <= self.s) & (self.s + 1 < self.n))
                def _():
                    self.right(there, o, c).wait_send()

                @pl.when((o >= self.s) & (self.s > 0))
                def _():
                    self.left(there, o, c).wait_send()

                @pl.when(o != self.s)
                def _():
                    self.twin(o, c, self.g).wait_send()


def greet_line():
    n, s, g = lax.axis_size("sp"), lax.axis_index("sp"), lax.axis_index("grp")
    barrier = pltpu.get_barrier_semaphore()
    pl.semaphore_signal(barrier, inc=1, device_id={"grp": 1 - g}, device_id_type=MESH)

    @pl.when(s + 1 < n)
    def _():
        pl.semaphore_signal(barrier, inc=1, device_id={"sp": lax.rem(s + 1, n)}, device_id_type=MESH)

    @pl.when(s > 0)
    def _():
        pl.semaphore_signal(barrier, inc=1, device_id={"sp": lax.rem(s + n - 1, n)}, device_id_type=MESH)

    pl.semaphore_wait(barrier, 1 + (s + 1 < n).astype(jnp.int32) + (s > 0).astype(jnp.int32))


def project_kernel(x_ref, w_ref, wo_ref, proj_ref, wo_all, wbuf, *sems):
    s = lax.axis_index("sp")
    depth = w_ref.shape[0]
    into = LineGather(w_ref, wbuf, *sems[:5])
    out = LineGather(wo_ref, wo_all, *sems[5:])
    greet_line()
    into.start()

    def columns(o):
        return pl.ds(pl.multiple_of(o * depth, depth), depth)

    proj_ref[...] = jnp.dot(x_ref[:, columns(s)], w_ref[...], preferred_element_type=jnp.float32)

    def add(o):
        proj_ref[...] += jnp.dot(x_ref[:, columns(o)], wbuf[o], preferred_element_type=jnp.float32)

    into.run(add)
    out.start()
    wo_all[s] = wo_ref[...]
    out.run(lambda o: None)
    into.finish()
    out.finish()


def gather_sems(n, chunks):
    return [pltpu.SemaphoreType.DMA((n, chunks)) for _ in range(5)]


def project(normed, weight, weight_out):
    n = lax.axis_size("sp")
    chunks = 4 if n <= 4 else 1
    return pl.pallas_call(
        project_kernel,
        out_shape=(
            jax.ShapeDtypeStruct((normed.shape[0], weight.shape[1]), jnp.float32),
            jax.ShapeDtypeStruct((n,) + weight_out.shape, jnp.bfloat16),
        ),
        in_specs=[pl.BlockSpec(memory_space=pltpu.VMEM)] * 3,
        out_specs=[pl.BlockSpec(memory_space=pltpu.VMEM)] * 2,
        scratch_shapes=[pltpu.VMEM((n,) + weight.shape, jnp.bfloat16)]
        + gather_sems(n, chunks)
        + gather_sems(n, chunks),
        compiler_params=pltpu.CompilerParams(
            collective_id=0, has_side_effects=True, vmem_limit_bytes=60 * 1024 * 1024
        ),
    )(normed, weight, weight_out)


def local(
    tokens_in,
    norm_gain,
    window_query,
    window_key,
    window_value,
    window_query_gain,
    window_key_gain,
    sink_logit,
    dense_query,
    dense_key,
    dense_value,
    dense_query_gain,
    dense_key_gain,
    window_out,
    dense_out,
):
    length = tokens_in.shape[0]
    inputs = tokens_in.astype(jnp.float32)
    normed = (
        inputs * lax.rsqrt(jnp.mean(inputs * inputs, axis=-1, keepdims=True) + EPS) * norm_gain
    ).astype(jnp.bfloat16)
    weights = (window_query, window_key, window_value, dense_query, dense_key, dense_value)
    weight_out = jnp.concatenate([window_out, dense_out], axis=0)
    joined, out_all = project(normed, jnp.concatenate(weights, axis=1), weight_out)
    projected, at = [], 0
    for weight in weights:
        projected.append(joined[:, at : at + weight.shape[1]])
        at += weight.shape[1]
    offset = lax.axis_index("sp") * length
    total_len = length * lax.axis_size("sp")
    places = offset + jnp.arange(length, dtype=jnp.int32)
    query_win = line_heads(projected[0], window_query_gain, places)
    key_win = line_heads(projected[1], window_key_gain, places)
    value_win = projected[2].astype(jnp.bfloat16)
    query_den = grid_heads(projected[3], dense_query_gain, places)
    key_den = grid_heads(projected[4], dense_key_gain, places)
    value_den = projected[5].astype(jnp.bfloat16)
    framed = extended(jnp.stack([key_win, value_win]), (("sp", 1),), WINDOW)
    att_win = banded(query_win, framed[0], framed[1], offset, total_len, sink_logit)
    dense_pair = jnp.stack([key_den, value_den])
    every = lax.all_gather(dense_pair, "sp", axis=1, tiled=True)
    att_den = dense_whole(query_den, every[0], every[1])
    att = jnp.concatenate([att_win, att_den], axis=1)
    terms = jnp.einsum("tk,nkc->tnc", att, out_all, preferred_element_type=jnp.float32)
    terms = terms.reshape(length, -1)
    rounded = lax.optimization_barrier(terms.astype(jnp.bfloat16)).astype(jnp.float32)
    return lax.psum_scatter(rounded.astype(jnp.bfloat16), "tp", scatter_dimension=0, tiled=True)


def solution(mesh):
    return jax.shard_map(
        local,
        mesh=mesh,
        in_specs=(
            P(("grp", "sp"), None),
            P(),
            P("sp", "tp"),
            P("sp", "tp"),
            P("sp", "tp"),
            P(),
            P(),
            P("tp"),
            P("sp", "tp"),
            P("sp", "tp"),
            P("sp", "tp"),
            P(),
            P(),
            P("tp", "sp"),
            P("tp", "sp"),
        ),
        out_specs=P(("grp", "sp", "tp"), None),
        check_vma=False,
    )
```

```python
import functools

import jax
import jax.numpy as jnp
from jax import lax
from jax.experimental import pallas as pl
from jax.experimental.pallas import tpu as pltpu
from jax.sharding import PartitionSpec as P

HD = 64
WINDOW = 128
GRID_W = 64


EPS = 1e-06
THETA = 10000.0


def rope_table(places, width):
    inverse = THETA ** (-jnp.arange(0, width, 2, dtype=jnp.float32) / width)
    angles = places.astype(jnp.float32)[:, None] * inverse[None, :]
    angles = jnp.concatenate([angles, angles], axis=-1)
    return (jnp.cos(angles), jnp.sin(angles))


MESH = pl.DeviceIdType.MESH
HALVES = 2


class LineGather:
    def __init__(self, own, buf, z_recv, r_send, l_send, y_recv=None, y_send=None):
        self.own, self.buf = own, buf
        self.z_recv, self.y_recv = z_recv, y_recv
        self.r_send, self.l_send, self.y_send = r_send, l_send, y_send
        self.n = lax.axis_size("sp")
        self.s = lax.axis_index("sp")
        self.shared = y_recv is not None
        self.g = lax.axis_index("grp") if self.shared else 0
        self.chunks = z_recv.shape[1]
        self.half = buf.shape[1] // HALVES if self.shared else buf.shape[1]
        self.size = self.half // self.chunks

    def rows(self, half, c):
        return pl.ds(pl.multiple_of(half * self.half + c * self.size, self.size), self.size)

    def copy(self, src, o, c, sem, recv, target, half):
        return pltpu.make_async_remote_copy(
            src_ref=src,
            dst_ref=self.buf.at[o, self.rows(half, c)],
            send_sem=sem.at[o, c],
            recv_sem=recv.at[o, c],
            device_id=target,
            device_id_type=MESH,
        )

    def right(self, src, o, c):
        return self.copy(src, o, c, self.r_send, self.z_recv, {"sp": lax.rem(self.s + 1, self.n)}, self.g)

    def left(self, src, o, c):
        return self.copy(
            src, o, c, self.l_send, self.z_recv, {"sp": lax.rem(self.s + self.n - 1, self.n)}, self.g
        )

    def twin(self, o, c, half):
        return self.copy(
            self.buf.at[o, self.rows(half, c)], o, c, self.y_send, self.y_recv, {"grp": 1 - self.g}, half
        )

    def mine(self, c):
        if self.own is None:
            return self.buf.at[self.s, self.rows(self.g, c)]
        return self.own.at[self.rows(self.g, c)]

    def start(self):
        for c in range(self.chunks):
            mine = self.mine(c)

            @pl.when(self.s + 1 < self.n)
            def _():
                self.right(mine, self.s, c).start()

            @pl.when(self.s > 0)
            def _():
                self.left(mine, self.s, c).start()

    def forward(self, d):
        for c in range(self.chunks):

            @pl.when(self.s - d >= 0)
            def _():
                o = self.s - d
                there = self.buf.at[o, self.rows(self.g, c)]
                self.right(there, o, c).wait_recv()

                @pl.when(self.s + 1 < self.n)
                def _():
                    self.right(there, o, c).start()

                if self.shared:
                    self.twin(o, c, self.g).start()

            @pl.when(self.s + d < self.n)
            def _():
                o = self.s + d
                there = self.buf.at[o, self.rows(self.g, c)]
                self.left(there, o, c).wait_recv()

                @pl.when(self.s > 0)
                def _():
                    self.left(there, o, c).start()

                if self.shared:
                    self.twin(o, c, self.g).start()

    def use(self, d, fn):
        @pl.when(self.s - d >= 0)
        def _():
            for c in range(self.chunks):
                self.twin(self.s - d, c, 1 - self.g).wait_recv()
            fn(self.s - d)

        @pl.when(self.s + d < self.n)
        def _():
            for c in range(self.chunks):
                self.twin(self.s + d, c, 1 - self.g).wait_recv()
            fn(self.s + d)

    def run(self, fn):
        self.forward(1)

        @pl.loop(2, self.n)
        def _(d):
            self.forward(d)
            self.use(d - 1, fn)

        self.use(self.n - 1, fn)

    def finish(self):
        @pl.loop(0, self.n)
        def _(o):
            for c in range(self.chunks):
                there = self.buf.at[o, self.rows(self.g, c)]

                @pl.when((o <= self.s) & (self.s + 1 < self.n))
                def _():
                    self.right(there, o, c).wait_send()

                @pl.when((o >= self.s) & (self.s > 0))
                def _():
                    self.left(there, o, c).wait_send()

                if self.shared:

                    @pl.when(o != self.s)
                    def _():
                        self.twin(o, c, self.g).wait_send()


def greet():
    n, s, g = lax.axis_size("sp"), lax.axis_index("sp"), lax.axis_index("grp")
    n_tp, t = lax.axis_size("tp"), lax.axis_index("tp")
    barrier = pltpu.get_barrier_semaphore()
    pl.semaphore_signal(barrier, inc=1, device_id={"grp": 1 - g}, device_id_type=MESH)
    for j in range(1, n_tp):
        pl.semaphore_signal(barrier, inc=1, device_id={"tp": lax.rem(t + j, n_tp)}, device_id_type=MESH)

    @pl.when(s + 1 < n)
    def _():
        pl.semaphore_signal(barrier, inc=1, device_id={"sp": lax.rem(s + 1, n)}, device_id_type=MESH)

    @pl.when(s > 0)
    def _():
        pl.semaphore_signal(barrier, inc=1, device_id={"sp": lax.rem(s + n - 1, n)}, device_id_type=MESH)

    pl.semaphore_wait(barrier, n_tp + (s + 1 < n).astype(jnp.int32) + (s > 0).astype(jnp.int32))


LANES = 128


def by_half(low, high):
    lane = lax.broadcasted_iota(jnp.int32, low.shape, 1)
    return jnp.where(lane < HD, low, high)


def swap_pairs(values, reach):
    lane = lax.broadcasted_iota(jnp.int32, values.shape, 1)
    ahead = pltpu.roll(values, LANES - reach, 1)
    behind = pltpu.roll(values, reach, 1)
    return jnp.where(lax.rem(lane, 2 * reach) < reach, ahead, behind)


def head_tile(tile, kinds, gains_ref, tables_ref):
    square = tile * tile
    zero = jnp.zeros_like(square)
    low = jnp.sum(by_half(square, zero), axis=-1, keepdims=True)
    high = jnp.sum(by_half(zero, square), axis=-1, keepdims=True)
    mean = by_half(jnp.broadcast_to(low, tile.shape), jnp.broadcast_to(high, tile.shape)) * (1.0 / HD)
    scaled = tile * lax.rsqrt(mean + EPS)

    def one(kind):
        if kind is None:
            return tile
        gain, table, reach = kind
        normed = scaled * gains_ref[gain : gain + 1, :]
        return normed * tables_ref[2 * table] + swap_pairs(normed, reach) * tables_ref[2 * table + 1]

    if kinds[0] == kinds[1]:
        return one(kinds[0])
    return by_half(one(kinds[0]), one(kinds[1]))


def layer_kernel(
    sizes, x_ref, gain_ref, w_ref, wo_ref, gains_ref, tables_ref, sink_ref, out_ref,
    xn, proj, wbuf, wo_all, kvd, ext, qs, att, part, rs, halo_recv, halo_send, rs_recv, rs_send, *sems
):
    q_heads, kv_heads = sizes
    n, s = lax.axis_size("sp"), lax.axis_index("sp")
    n_tp, t = lax.axis_size("tp"), lax.axis_index("tp")
    depth = w_ref.shape[0]
    length = x_ref.shape[0]
    into = LineGather(w_ref, wbuf, *sems[:5])
    out = LineGather(wo_ref, wo_all, *sems[5:10])
    keys = LineGather(None, kvd, *sems[10:])
    greet()
    into.start()

    step = 16

    @pl.loop(0, length // step)
    def _(i):
        rows = pl.ds(pl.multiple_of(i * step, step), step)
        values = x_ref[rows, :].astype(jnp.float32)
        mean = jnp.mean(values * values, axis=-1, keepdims=True)
        xn[rows, :] = (values * lax.rsqrt(mean + EPS) * gain_ref[...]).astype(jnp.bfloat16)

    def columns(o):
        return pl.ds(pl.multiple_of(o * depth, depth), depth)

    proj[...] = jnp.dot(xn[:, columns(s)], w_ref[...], preferred_element_type=jnp.float32)

    def add(o):
        proj[...] += jnp.dot(xn[:, columns(o)], wbuf[o], preferred_element_type=jnp.float32)

    into.run(add)

    win_q, win_k, den_q, den_k = (0, 0, 32), (1, 0, 32), (2, 1, 16), (3, 1, 16)
    kinds = (
        [win_q] * q_heads + [den_q] * q_heads + [den_k] * kv_heads + [None] * kv_heads
        + [win_k] * kv_heads + [None] * kv_heads
    )
    q_tiles = 2 * q_heads * HD // LANES
    kv_tiles = 2 * kv_heads * HD // LANES

    def finished(i):
        return head_tile(
            proj[:, i * LANES : (i + 1) * LANES], kinds[2 * i : 2 * i + 2], gains_ref, tables_ref
        )

    for i in range(kv_tiles):
        ext[WINDOW : WINDOW + length, i * LANES : (i + 1) * LANES] = finished(
            q_tiles + kv_tiles + i
        ).astype(jnp.bfloat16)
    for i in range(kv_tiles):
        kvd[s, :, i * LANES : (i + 1) * LANES] = finished(q_tiles + i).astype(jnp.bfloat16)

    def halo(side):
        source = pl.ds(length, WINDOW) if side == 0 else pl.ds(WINDOW, WINDOW)
        target = pl.ds(0, WINDOW) if side == 0 else pl.ds(WINDOW + length, WINDOW)
        peer = lax.rem(s + 1, n) if side == 0 else lax.rem(s + n - 1, n)
        return pltpu.make_async_remote_copy(
            src_ref=ext.at[source], dst_ref=ext.at[target], send_sem=halo_send.at[side],
            recv_sem=halo_recv.at[side], device_id={"sp": peer}, device_id_type=MESH,
        )

    has_right, has_left = s + 1 < n, s > 0

    @pl.when(has_right)
    def _():
        halo(0).start()

    @pl.when(has_left)
    def _():
        halo(1).start()

    keys.start()
    none = jnp.zeros((WINDOW, ext.shape[1]), jnp.bfloat16)

    @pl.when(jnp.logical_not(has_left))
    def _():
        ext[0:WINDOW, :] = none

    @pl.when(jnp.logical_not(has_right))
    def _():
        ext[WINDOW + length : WINDOW + length + WINDOW, :] = none

    group = q_heads // kv_heads

    def place(head):
        return head // 2, head % 2

    for i in range(q_tiles):
        tile = finished(i) * HD ** (-0.5)
        for b in range(2):
            head = 2 * i + b
            half = place((head % q_heads) // group)[1]
            moved = tile if half == b else pltpu.roll(tile, HD, 1)
            zero = jnp.zeros_like(moved)
            kept = by_half(moved, zero) if half == 0 else by_half(zero, moved)
            qs[head] = kept.astype(jnp.bfloat16)

    @pl.when(has_left)
    def _():
        halo(0).wait_recv()

    @pl.when(has_right)
    def _():
        halo(1).wait_recv()

    total_len = length * n

    def joined(results, heads):
        placed = []
        for b in range(2):
            half = place(kv_heads + heads[b] // group)[1]
            placed.append(results[b] if half == b else pltpu.roll(results[b], HD, 1))
        return by_half(placed[0], placed[1]).astype(jnp.bfloat16)

    def tile_of(head):
        return pl.ds(place(head)[0] * LANES, LANES)

    nt = (((1,), (1,)), ((), ()))

    def windowed(pair):
        @pl.loop(0, length // WINDOW)
        def _(b):
            base = pl.multiple_of(b * WINDOW, WINDOW)
            rows = pl.ds(base, WINDOW)
            near = pl.ds(base, 3 * WINDOW)
            shape = (WINDOW, 3 * WINDOW)
            at = lax.broadcasted_iota(jnp.int32, shape, 1) - WINDOW
            away = at - lax.broadcasted_iota(jnp.int32, shape, 0)
            pos = at + (s * length + base)
            valid = (away <= WINDOW) & (away >= -WINDOW) & (pos >= 0) & (pos < total_len)
            results = []
            for head in (2 * pair, 2 * pair + 1):
                key = ext[near, tile_of(head // group)]
                value = ext[near, tile_of(kv_heads + head // group)]
                scores = lax.dot_general(qs[head, rows, :], key, nt, preferred_element_type=jnp.float32)
                scores = jnp.where(valid, scores, -jnp.inf)
                floor = sink_ref[0, head]
                top = jnp.maximum(jnp.max(scores, axis=-1, keepdims=True), floor)
                expon = jnp.exp(scores - top)
                total = jnp.sum(expon, axis=-1, keepdims=True) + jnp.exp(floor - top)
                weights = (expon / total).astype(jnp.bfloat16)
                results.append(jnp.dot(weights, value, preferred_element_type=jnp.float32))
            att[rows, pair * LANES : (pair + 1) * LANES] = joined(results, (2 * pair, 2 * pair + 1))

    pairs = q_heads // 2
    keys.forward(1)
    windowed(0)

    @pl.loop(2, n)
    def _(d):
        keys.forward(d)

    out.start()
    for pair in range(1, pairs):
        windowed(pair)

    def dense(pair):
        @pl.loop(0, length // LANES)
        def _(b):
            rows = pl.ds(pl.multiple_of(b * LANES, LANES), LANES)
            results = []
            for head in (2 * pair, 2 * pair + 1):
                key = kvd[:, :, tile_of(head // group)].reshape(total_len, LANES)
                value = kvd[:, :, tile_of(kv_heads + head // group)].reshape(total_len, LANES)
                scores = lax.dot_general(
                    qs[q_heads + head, rows, :], key, nt, preferred_element_type=jnp.float32
                )
                top = jnp.max(scores, axis=-1, keepdims=True)
                expon = jnp.exp(scores - top)
                total = jnp.sum(expon, axis=-1, keepdims=True)
                summed = jnp.dot(
                    expon.astype(jnp.bfloat16), value, preferred_element_type=jnp.float32
                )
                results.append(summed / total)
            at = (pairs + pair) * LANES
            att[rows, at : at + LANES] = joined(results, (2 * pair, 2 * pair + 1))

    for pair in range(pairs):
        dense(pair)

    share = length // n_tp

    def exchange(o, j):
        peer = lax.rem(t + j, n_tp)
        return pltpu.make_async_remote_copy(
            src_ref=part.at[o, pl.ds(pl.multiple_of(peer * share, share), share)],
            dst_ref=rs.at[t, o], send_sem=rs_send.at[j - 1, o],
            recv_sem=rs_recv.at[t, o], device_id={"tp": peer}, device_id_type=MESH,
        )

    def arrived(o, j):
        source = lax.rem(t + n_tp - j, n_tp)
        return pltpu.make_async_remote_copy(
            src_ref=rs.at[source, o], dst_ref=rs.at[source, o], send_sem=rs_send.at[j - 1, o],
            recv_sem=rs_recv.at[source, o], device_id={"tp": source}, device_id_type=MESH,
        )

    def emit(o, weight):
        part[o] = jnp.dot(att[...], weight, preferred_element_type=jnp.float32).astype(jnp.bfloat16)
        rs[t, o] = part[o, pl.ds(pl.multiple_of(t * share, share), share), :]
        for j in range(1, n_tp):
            exchange(o, j).start()

    def collect(o):
        for j in range(1, n_tp):
            arrived(o, j).wait_recv()
        total = rs[0, o].astype(jnp.float32)
        for g in range(1, n_tp):
            total += rs[g, o].astype(jnp.float32)
        wide = wo_ref.shape[1]
        out_ref[:, pl.ds(pl.multiple_of(o * wide, wide), wide)] = total.astype(jnp.bfloat16)

    emit(s, wo_ref[...])
    out.run(lambda o: emit(o, wo_all[o]))

    @pl.loop(0, n)
    def _(o):
        collect(o)

    @pl.loop(0, n)
    def _(o):
        for j in range(1, n_tp):
            exchange(o, j).wait_send()

    @pl.when(has_right)
    def _():
        halo(0).wait_send()

    @pl.when(has_left)
    def _():
        halo(1).wait_send()

    into.finish()
    out.finish()
    keys.finish()


def local(
    tokens_in,
    norm_gain,
    window_query,
    window_key,
    window_value,
    window_query_gain,
    window_key_gain,
    sink_logit,
    dense_query,
    dense_key,
    dense_value,
    dense_query_gain,
    dense_key_gain,
    window_out,
    dense_out,
):
    length, width = tokens_in.shape
    n, n_tp = lax.axis_size("sp"), lax.axis_size("tp")
    q_heads, kv_heads = window_query.shape[1] // HD, window_key.shape[1] // HD
    weight = jnp.concatenate(
        (window_query, dense_query, dense_key, dense_value, window_key, window_value), axis=1
    )
    weight_out = jnp.concatenate((window_out, dense_out), axis=0)
    gains = jnp.stack(
        [jnp.tile(g, 2) for g in (window_query_gain, window_key_gain, dense_query_gain, dense_key_gain)]
    )
    places = lax.axis_index("sp") * length + jnp.arange(length, dtype=jnp.int32)
    signs = jnp.where(jnp.arange(HD) < HD // 2, -1.0, 1.0)
    cosine, sine = rope_table(places, HD)
    tables = [cosine, sine * signs]
    quarter = jnp.where(jnp.arange(HD // 2) < HD // 4, -1.0, 1.0)
    row_cos, row_sin = rope_table(places // GRID_W, HD // 2)
    col_cos, col_sin = rope_table(places % GRID_W, HD // 2)
    tables.append(jnp.concatenate([row_cos, col_cos], axis=1))
    tables.append(jnp.concatenate([row_sin * quarter, col_sin * quarter], axis=1))
    tables = jnp.stack([jnp.concatenate([table, table], axis=1) for table in tables])
    chunks = 4 if n <= 4 else 1
    gather = [pltpu.SemaphoreType.DMA((n, chunks)) for _ in range(5)]
    kv_cols = 2 * kv_heads * HD
    vmem = pl.BlockSpec(memory_space=pltpu.VMEM)
    share = length // n_tp
    return pl.pallas_call(
        functools.partial(layer_kernel, (q_heads, kv_heads)),
        out_shape=jax.ShapeDtypeStruct((share, width), jnp.bfloat16),
        in_specs=[vmem] * 6 + [pl.BlockSpec(memory_space=pltpu.SMEM)],
        out_specs=vmem,
        scratch_shapes=[
            pltpu.VMEM((length, width), jnp.bfloat16),
            pltpu.VMEM((length, weight.shape[1]), jnp.float32),
            pltpu.VMEM((n,) + weight.shape, jnp.bfloat16),
            pltpu.VMEM((n,) + weight_out.shape, jnp.bfloat16),
            pltpu.VMEM((n, length, kv_cols), jnp.bfloat16),
            pltpu.VMEM((length + 2 * WINDOW, kv_cols), jnp.bfloat16),
            pltpu.VMEM((2 * q_heads, length, LANES), jnp.bfloat16),
            pltpu.VMEM((length, weight_out.shape[0]), jnp.bfloat16),
            pltpu.VMEM((n, length, weight_out.shape[1]), jnp.bfloat16),
            pltpu.VMEM((n_tp, n, share, weight_out.shape[1]), jnp.bfloat16),
            pltpu.SemaphoreType.DMA((2,)),
            pltpu.SemaphoreType.DMA((2,)),
            pltpu.SemaphoreType.DMA((n_tp, n)),
            pltpu.SemaphoreType.DMA((n_tp - 1, n)),
        ]
        + gather
        + gather
        + [pltpu.SemaphoreType.DMA((n, 2 if n <= 4 else 1)) for _ in range(3)],
        compiler_params=pltpu.CompilerParams(
            collective_id=0, has_side_effects=True, vmem_limit_bytes=62 * 1024 * 1024
        ),
    )(tokens_in, norm_gain[None, :], weight, weight_out, gains, tables, sink_logit[None, :])


def solution(mesh):
    return jax.shard_map(
        local,
        mesh=mesh,
        in_specs=(
            P(("grp", "sp"), None),
            P(),
            P("sp", "tp"),
            P("sp", "tp"),
            P("sp", "tp"),
            P(),
            P(),
            P("tp"),
            P("sp", "tp"),
            P("sp", "tp"),
            P("sp", "tp"),
            P(),
            P(),
            P("tp", "sp"),
            P("tp", "sp"),
        ),
        out_specs=P(("grp", "sp", "tp"), None),
        check_vma=False,
    )
```

```python
import functools

import jax
import jax.numpy as jnp
from jax import lax
from jax.experimental import pallas as pl
from jax.experimental.pallas import tpu as pltpu
from jax.sharding import PartitionSpec as P

HD = 64
WINDOW = 128
GRID_W = 64


EPS = 1e-06
THETA = 10000.0


MESH = pl.DeviceIdType.MESH
HALVES = 2


class LineGather:
    def __init__(self, own, buf, z_recv, r_send, l_send, y_recv=None, y_send=None, axis=0):
        self.own, self.buf = own, buf
        self.z_recv, self.y_recv = z_recv, y_recv
        self.r_send, self.l_send, self.y_send = r_send, l_send, y_send
        self.n = lax.axis_size("sp")
        self.s = lax.axis_index("sp")
        self.shared = y_recv is not None
        self.g = lax.axis_index("grp") if self.shared else 0
        self.chunks = z_recv.shape[1]
        self.axis = axis
        extent = buf.shape[1 + axis]
        self.half = extent // HALVES if self.shared else extent
        self.size = self.half // self.chunks

    def rows(self, half, c):
        piece = pl.ds(pl.multiple_of(half * self.half + c * self.size, self.size), self.size)
        return (piece,) if self.axis == 0 else (slice(None), piece)

    def block(self, o, half, c):
        return self.buf.at[(o,) + self.rows(half, c)]

    def copy(self, src, o, c, sem, recv, target, half):
        return pltpu.make_async_remote_copy(
            src_ref=src,
            dst_ref=self.block(o, half, c),
            send_sem=sem.at[o, c],
            recv_sem=recv.at[o, c],
            device_id=target,
            device_id_type=MESH,
        )

    def right(self, src, o, c):
        return self.copy(src, o, c, self.r_send, self.z_recv, {"sp": lax.rem(self.s + 1, self.n)}, self.g)

    def left(self, src, o, c):
        return self.copy(
            src, o, c, self.l_send, self.z_recv, {"sp": lax.rem(self.s + self.n - 1, self.n)}, self.g
        )

    def twin(self, o, c, half):
        return self.copy(
            self.block(o, half, c), o, c, self.y_send, self.y_recv, {"grp": 1 - self.g}, half
        )

    def mine(self, c):
        if self.own is None:
            return self.block(self.s, self.g, c)
        return self.own.at[self.rows(self.g, c)]

    def start(self, first=0, last=None):
        for c in range(first, self.chunks if last is None else last):
            mine = self.mine(c)

            @pl.when(self.s + 1 < self.n)
            def _():
                self.right(mine, self.s, c).start()

            @pl.when(self.s > 0)
            def _():
                self.left(mine, self.s, c).start()

    def forward(self, d):
        for c in range(self.chunks):

            @pl.when(self.s - d >= 0)
            def _():
                o = self.s - d
                there = self.block(o, self.g, c)
                self.right(there, o, c).wait_recv()

                @pl.when(self.s + 1 < self.n)
                def _():
                    self.right(there, o, c).start()

                if self.shared:
                    self.twin(o, c, self.g).start()

            @pl.when(self.s + d < self.n)
            def _():
                o = self.s + d
                there = self.block(o, self.g, c)
                self.left(there, o, c).wait_recv()

                @pl.when(self.s > 0)
                def _():
                    self.left(there, o, c).start()

                if self.shared:
                    self.twin(o, c, self.g).start()

    def use(self, d, fn, near=None):
        for there, o in ((self.s - d >= 0, self.s - d), (self.s + d < self.n, self.s + d)):
            if near is not None:

                @pl.when(there)
                def _():
                    near(o)

        for there, o in ((self.s - d >= 0, self.s - d), (self.s + d < self.n, self.s + d)):

            @pl.when(there)
            def _():
                for c in range(self.chunks):
                    self.twin(o, c, 1 - self.g).wait_recv()
                fn(o)

    def run(self, fn, near=None, last=None):
        self.forward(1)

        @pl.loop(2, self.n)
        def _(d):
            self.forward(d)
            self.use(d - 1, fn, near)

        if last is not None:
            last()
        self.use(self.n - 1, fn, near)

    def finish(self):
        @pl.loop(0, self.n)
        def _(o):
            for c in range(self.chunks):
                there = self.block(o, self.g, c)

                @pl.when((o <= self.s) & (self.s + 1 < self.n))
                def _():
                    self.right(there, o, c).wait_send()

                @pl.when((o >= self.s) & (self.s > 0))
                def _():
                    self.left(there, o, c).wait_send()

                if self.shared:

                    @pl.when(o != self.s)
                    def _():
                        self.twin(o, c, self.g).wait_send()


def greet():
    n, s, g = lax.axis_size("sp"), lax.axis_index("sp"), lax.axis_index("grp")
    n_tp, t = lax.axis_size("tp"), lax.axis_index("tp")
    barrier = pltpu.get_barrier_semaphore()
    pl.semaphore_signal(barrier, inc=1, device_id={"grp": 1 - g}, device_id_type=MESH)
    for j in range(1, n_tp):
        pl.semaphore_signal(barrier, inc=1, device_id={"tp": lax.rem(t + j, n_tp)}, device_id_type=MESH)

    @pl.when(s + 1 < n)
    def _():
        pl.semaphore_signal(barrier, inc=1, device_id={"sp": lax.rem(s + 1, n)}, device_id_type=MESH)

    @pl.when(s > 0)
    def _():
        pl.semaphore_signal(barrier, inc=1, device_id={"sp": lax.rem(s + n - 1, n)}, device_id_type=MESH)

    pl.semaphore_wait(barrier, n_tp + (s + 1 < n).astype(jnp.int32) + (s > 0).astype(jnp.int32))


LANES = 128


def by_half(low, high):
    lane = lax.broadcasted_iota(jnp.int32, low.shape, 1)
    return jnp.where(lane < HD, low, high)


def swap_pairs(values, reach):
    lane = lax.broadcasted_iota(jnp.int32, values.shape, 1)
    ahead = pltpu.roll(values, LANES - reach, 1)
    behind = pltpu.roll(values, reach, 1)
    return jnp.where(lax.rem(lane, 2 * reach) < reach, ahead, behind)


def head_tile(tile, kinds, gains_ref, tables_ref):
    square = tile * tile
    zero = jnp.zeros_like(square)
    low = jnp.sum(by_half(square, zero), axis=-1, keepdims=True)
    high = jnp.sum(by_half(zero, square), axis=-1, keepdims=True)
    mean = by_half(jnp.broadcast_to(low, tile.shape), jnp.broadcast_to(high, tile.shape)) * (1.0 / HD)
    scaled = tile * lax.rsqrt(mean + EPS)

    def one(kind):
        if kind is None:
            return tile
        gain, table, reach = kind
        normed = scaled * gains_ref[gain : gain + 1, :]
        return normed * tables_ref[2 * table] + swap_pairs(normed, reach) * tables_ref[2 * table + 1]

    if kinds[0] == kinds[1]:
        return one(kinds[0])
    return by_half(one(kinds[0]), one(kinds[1]))


def layer_kernel(
    sizes, x_ref, gain_ref, small_ref, sink_ref, *refs
):
    n_in = sizes[2]
    in_refs, out_refs = refs[:n_in], refs[n_in : n_in + 2]
    run_layer(sizes[:2], x_ref, gain_ref, small_ref, sink_ref, in_refs, out_refs, *refs[n_in + 2 :])


def run_layer(
    sizes, x_ref, gain_ref, small_ref, sink_ref, in_refs, out_refs, out_ref,
    w_ref, wo_ref, tables_ref, load_sem, xn, proj, wbuf, wo_all, kvd, ext, qs, att, part, rs, halo_recv, halo_send, rs_recv, rs_send, *sems
):
    q_heads, kv_heads = sizes
    n, s = lax.axis_size("sp"), lax.axis_index("sp")
    n_tp, t = lax.axis_size("tp"), lax.axis_index("tp")
    depth = w_ref.shape[0]
    length = x_ref.shape[0]
    into = LineGather(w_ref, wbuf, *sems[:5])
    out = LineGather(wo_ref, wo_all, *sems[5:10], axis=1)
    keys = LineGather(None, kvd, *sems[10:])
    loads, at = [], 0
    for ref in in_refs:
        wide = ref.shape[1]
        loads.append(
            pltpu.make_async_copy(ref, w_ref.at[:, at : at + wide], load_sem.at[len(loads)])
        )
        at += wide
    at = 0
    for ref in out_refs:
        tall = ref.shape[0]
        loads.append(pltpu.make_async_copy(ref, wo_ref.at[at : at + tall], load_sem.at[len(loads)]))
        at += tall
    for load in loads:
        load.start()
    greet()
    for load in loads:
        load.wait()
    into.start()

    step = 16

    @pl.loop(0, length // step)
    def _(i):
        rows = pl.ds(pl.multiple_of(i * step, step), step)
        values = x_ref[rows, :].astype(jnp.float32)
        mean = jnp.mean(values * values, axis=-1, keepdims=True)
        xn[rows, :] = (values * lax.rsqrt(mean + EPS) * gain_ref[...]).astype(jnp.bfloat16)

    def columns(o):
        return pl.ds(pl.multiple_of(o * depth, depth), depth)

    proj[...] = jnp.dot(xn[:, columns(s)], w_ref[...], preferred_element_type=jnp.float32)

    band = 64 if length % 64 == 0 else length

    @pl.loop(0, length // band)
    def _(i):
        rows = pl.ds(pl.multiple_of(i * band, band), band)
        shape = (band, LANES)
        place = lax.broadcasted_iota(jnp.int32, shape, 0) + (s * length + i * band)
        lane = lax.broadcasted_iota(jnp.int32, shape, 1)
        spot = jnp.where(lax.rem(lane, HD) < HD // 2, place // GRID_W, lax.rem(place, GRID_W))
        for k, where in enumerate((place, spot)):
            angles = where.astype(jnp.float32) * small_ref[4 + k : 5 + k, :]
            tables_ref[2 * k, rows, :] = jnp.cos(angles)
            tables_ref[2 * k + 1, rows, :] = jnp.sin(angles) * small_ref[6 + k : 7 + k, :]

    def add(o):
        proj[...] += jnp.dot(xn[:, columns(o)], wbuf[o], preferred_element_type=jnp.float32)

    into.run(add, last=lambda: out.start(0, 1))

    win_q, win_k, den_q, den_k = (0, 0, 32), (1, 0, 32), (2, 1, 16), (3, 1, 16)
    kinds = (
        [win_q] * q_heads + [den_q] * q_heads + [den_k] * kv_heads + [None] * kv_heads
        + [win_k] * kv_heads + [None] * kv_heads
    )
    q_tiles = 2 * q_heads * HD // LANES
    kv_tiles = 2 * kv_heads * HD // LANES

    def finished(i):
        return head_tile(
            proj[:, i * LANES : (i + 1) * LANES], kinds[2 * i : 2 * i + 2], small_ref, tables_ref
        )

    for i in range(kv_tiles):
        ext[WINDOW : WINDOW + length, i * LANES : (i + 1) * LANES] = finished(
            q_tiles + kv_tiles + i
        ).astype(jnp.bfloat16)
    for i in range(kv_tiles):
        kvd[s, :, i * LANES : (i + 1) * LANES] = finished(q_tiles + i).astype(jnp.bfloat16)

    def halo(side):
        source = pl.ds(length, WINDOW) if side == 0 else pl.ds(WINDOW, WINDOW)
        target = pl.ds(0, WINDOW) if side == 0 else pl.ds(WINDOW + length, WINDOW)
        peer = lax.rem(s + 1, n) if side == 0 else lax.rem(s + n - 1, n)
        return pltpu.make_async_remote_copy(
            src_ref=ext.at[source], dst_ref=ext.at[target], send_sem=halo_send.at[side],
            recv_sem=halo_recv.at[side], device_id={"sp": peer}, device_id_type=MESH,
        )

    has_right, has_left = s + 1 < n, s > 0

    @pl.when(has_right)
    def _():
        halo(0).start()

    @pl.when(has_left)
    def _():
        halo(1).start()

    keys.start()
    none = jnp.zeros((WINDOW, ext.shape[1]), jnp.bfloat16)

    @pl.when(jnp.logical_not(has_left))
    def _():
        ext[0:WINDOW, :] = none

    @pl.when(jnp.logical_not(has_right))
    def _():
        ext[WINDOW + length : WINDOW + length + WINDOW, :] = none

    group = q_heads // kv_heads

    def place(head):
        return head // 2, head % 2

    for i in range(q_tiles):
        tile = finished(i) * HD ** (-0.5)
        for b in range(2):
            head = 2 * i + b
            half = place((head % q_heads) // group)[1]
            moved = tile if half == b else pltpu.roll(tile, HD, 1)
            zero = jnp.zeros_like(moved)
            kept = by_half(moved, zero) if half == 0 else by_half(zero, moved)
            qs[head] = kept.astype(jnp.bfloat16)

    @pl.when(has_left)
    def _():
        halo(0).wait_recv()

    @pl.when(has_right)
    def _():
        halo(1).wait_recv()

    total_len = length * n

    def joined(results, heads):
        placed = []
        for b in range(2):
            half = place(kv_heads + heads[b] // group)[1]
            placed.append(results[b] if half == b else pltpu.roll(results[b], HD, 1))
        return by_half(placed[0], placed[1]).astype(jnp.bfloat16)

    def tile_of(head):
        return pl.ds(place(head)[0] * LANES, LANES)

    nt = (((1,), (1,)), ((), ()))

    def windowed(pair):
        @pl.loop(0, length // WINDOW)
        def _(b):
            base = pl.multiple_of(b * WINDOW, WINDOW)
            rows = pl.ds(base, WINDOW)
            near = pl.ds(base, 3 * WINDOW)
            shape = (WINDOW, 3 * WINDOW)
            at = lax.broadcasted_iota(jnp.int32, shape, 1) - WINDOW
            away = at - lax.broadcasted_iota(jnp.int32, shape, 0)
            pos = at + (s * length + base)
            valid = (away <= WINDOW) & (away >= -WINDOW) & (pos >= 0) & (pos < total_len)
            results = []
            for head in (2 * pair, 2 * pair + 1):
                key = ext[near, tile_of(head // group)]
                value = ext[near, tile_of(kv_heads + head // group)]
                scores = lax.dot_general(qs[head, rows, :], key, nt, preferred_element_type=jnp.float32)
                scores = jnp.where(valid, scores, -jnp.inf)
                floor = sink_ref[0, head]
                top = jnp.maximum(jnp.max(scores, axis=-1, keepdims=True), floor)
                expon = jnp.exp(scores - top)
                total = jnp.sum(expon, axis=-1, keepdims=True) + jnp.exp(floor - top)
                weights = (expon / total).astype(jnp.bfloat16)
                results.append(jnp.dot(weights, value, preferred_element_type=jnp.float32))
            att[rows, pair * LANES : (pair + 1) * LANES] = joined(results, (2 * pair, 2 * pair + 1))

    pairs = q_heads // 2
    keys.forward(1)
    windowed(0)

    @pl.loop(2, n)
    def _(d):
        keys.forward(d)

    out.start(1)
    for pair in range(1, pairs):
        windowed(pair)

    def dense(pair):
        @pl.loop(0, length // LANES)
        def _(b):
            rows = pl.ds(pl.multiple_of(b * LANES, LANES), LANES)
            results = []
            for head in (2 * pair, 2 * pair + 1):
                key = kvd[:, :, tile_of(head // group)].reshape(total_len, LANES)
                value = kvd[:, :, tile_of(kv_heads + head // group)].reshape(total_len, LANES)
                scores = lax.dot_general(
                    qs[q_heads + head, rows, :], key, nt, preferred_element_type=jnp.float32
                )
                top = jnp.max(scores, axis=-1, keepdims=True)
                expon = jnp.exp(scores - top)
                total = jnp.sum(expon, axis=-1, keepdims=True)
                summed = jnp.dot(
                    expon.astype(jnp.bfloat16), value, preferred_element_type=jnp.float32
                )
                results.append(summed / total)
            at = (pairs + pair) * LANES
            att[rows, at : at + LANES] = joined(results, (2 * pair, 2 * pair + 1))

    for pair in range(pairs):
        dense(pair)

    share = length // n_tp

    wide = wo_ref.shape[1]
    part_cols = wide // HALVES
    mine = lax.axis_index("grp")

    def span(h):
        return pl.ds(pl.multiple_of(h * part_cols, part_cols), part_cols)

    def exchange(o, h, j):
        peer = lax.rem(t + j, n_tp)
        return pltpu.make_async_remote_copy(
            src_ref=part.at[o, pl.ds(pl.multiple_of(peer * share, share), share), span(h)],
            dst_ref=rs.at[t, o, :, span(h)], send_sem=rs_send.at[j - 1, o, h],
            recv_sem=rs_recv.at[t, o, h], device_id={"tp": peer}, device_id_type=MESH,
        )

    def arrived(o, h, j):
        source = lax.rem(t + n_tp - j, n_tp)
        there = rs.at[source, o, :, span(h)]
        return pltpu.make_async_remote_copy(
            src_ref=there, dst_ref=there, send_sem=rs_send.at[j - 1, o, h],
            recv_sem=rs_recv.at[source, o, h], device_id={"tp": source}, device_id_type=MESH,
        )

    def emit(o, h, weight):
        part[o, :, span(h)] = jnp.dot(
            att[...], weight, preferred_element_type=jnp.float32
        ).astype(jnp.bfloat16)
        for j in range(1, n_tp):
            exchange(o, h, j).start()
        rs[t, o, :, span(h)] = part[o, pl.ds(pl.multiple_of(t * share, share), share), span(h)]

    def collect(o, h):
        for j in range(1, n_tp):
            arrived(o, h, j).wait_recv()
        total = rs[0, o, :, span(h)].astype(jnp.float32)
        for g in range(1, n_tp):
            total += rs[g, o, :, span(h)].astype(jnp.float32)
        columns_out = pl.ds(pl.multiple_of(o * wide + h * part_cols, part_cols), part_cols)
        out_ref[:, columns_out] = total.astype(jnp.bfloat16)

    for h in range(HALVES):
        emit(s, h, wo_ref[:, span(h)])
    out.run(
        lambda o: emit(o, 1 - mine, wo_all[o, :, span(1 - mine)]),
        near=lambda o: emit(o, mine, wo_all[o, :, span(mine)]),
    )

    @pl.loop(0, n)
    def _(d):
        o = lax.rem(s + d, n)
        for h in range(HALVES):
            collect(o, h)

    @pl.loop(0, n)
    def _(o):
        for h in range(HALVES):
            for j in range(1, n_tp):
                exchange(o, h, j).wait_send()

    @pl.when(has_right)
    def _():
        halo(0).wait_send()

    @pl.when(has_left)
    def _():
        halo(1).wait_send()

    into.finish()
    out.finish()
    keys.finish()


def local(
    tokens_in,
    norm_gain,
    window_query,
    window_key,
    window_value,
    window_query_gain,
    window_key_gain,
    sink_logit,
    dense_query,
    dense_key,
    dense_value,
    dense_query_gain,
    dense_key_gain,
    window_out,
    dense_out,
):
    length, width = tokens_in.shape
    n, n_tp = lax.axis_size("sp"), lax.axis_size("tp")
    q_heads, kv_heads = window_query.shape[1] // HD, window_key.shape[1] // HD
    weights, held = [], []
    for weight in (window_query, dense_query, dense_key, dense_value, window_key, window_value):
        held.append(weight)
        if sum(w.shape[1] for w in held) % LANES == 0:
            weights.append(held[0] if len(held) == 1 else jnp.concatenate(held, axis=1))
            held = []
    depth, in_cols = window_query.shape[0], sum(w.shape[1] for w in weights)
    out_rows, out_cols = window_out.shape[0] + dense_out.shape[0], window_out.shape[1]

    def lanes(row):
        return jnp.tile(row, LANES // row.shape[0])[None, :]

    def inverse(wide):
        return THETA ** (-jnp.arange(0, wide, 2, dtype=jnp.float32) / wide)

    def signs(wide):
        return jnp.where(jnp.arange(wide) < wide // 2, -1.0, 1.0).astype(jnp.float32)

    small = jnp.concatenate(
        [
            lanes(window_query_gain),
            lanes(window_key_gain),
            lanes(dense_query_gain),
            lanes(dense_key_gain),
            lanes(inverse(HD)),
            lanes(inverse(HD // 2)),
            lanes(signs(HD)),
            lanes(signs(HD // 2)),
        ],
        axis=0,
    )
    def gather(chunks):
        return [pltpu.SemaphoreType.DMA((n, chunks)) for _ in range(5)]

    in_chunks = 8 if n <= 4 else 1
    out_chunks = out_cols // HALVES // LANES if n <= 4 else 1
    kv_cols = 2 * kv_heads * HD
    vmem = pl.BlockSpec(memory_space=pltpu.VMEM)
    share = length // n_tp
    return pl.pallas_call(
        functools.partial(layer_kernel, (q_heads, kv_heads, len(weights))),
        out_shape=jax.ShapeDtypeStruct((share, width), jnp.bfloat16),
        in_specs=[vmem] * 3
        + [pl.BlockSpec(memory_space=pltpu.SMEM)]
        + [pl.BlockSpec(memory_space=pl.ANY)] * (len(weights) + 2),
        out_specs=vmem,
        scratch_shapes=[
            pltpu.VMEM((depth, in_cols), jnp.bfloat16),
            pltpu.VMEM((out_rows, out_cols), jnp.bfloat16),
            pltpu.VMEM((4, length, LANES), jnp.float32),
            pltpu.SemaphoreType.DMA((len(weights) + 2,)),
            pltpu.VMEM((length, width), jnp.bfloat16),
            pltpu.VMEM((length, in_cols), jnp.float32),
            pltpu.VMEM((n, depth, in_cols), jnp.bfloat16),
            pltpu.VMEM((n, out_rows, out_cols), jnp.bfloat16),
            pltpu.VMEM((n, length, kv_cols), jnp.bfloat16),
            pltpu.VMEM((length + 2 * WINDOW, kv_cols), jnp.bfloat16),
            pltpu.VMEM((2 * q_heads, length, LANES), jnp.bfloat16),
            pltpu.VMEM((length, out_rows), jnp.bfloat16),
            pltpu.VMEM((n, length, out_cols), jnp.bfloat16),
            pltpu.VMEM((n_tp, n, share, out_cols), jnp.bfloat16),
            pltpu.SemaphoreType.DMA((2,)),
            pltpu.SemaphoreType.DMA((2,)),
            pltpu.SemaphoreType.DMA((n_tp, n, HALVES)),
            pltpu.SemaphoreType.DMA((n_tp - 1, n, HALVES)),
        ]
        + gather(in_chunks)
        + gather(out_chunks)
        + [pltpu.SemaphoreType.DMA((n, 2 if n <= 4 else 1)) for _ in range(3)],
        compiler_params=pltpu.CompilerParams(
            collective_id=0, has_side_effects=True, vmem_limit_bytes=62 * 1024 * 1024
        ),
    )(tokens_in, norm_gain[None, :], small, sink_logit[None, :], *weights, window_out, dense_out)


def solution(mesh):
    return jax.shard_map(
        local,
        mesh=mesh,
        in_specs=(
            P(("grp", "sp"), None),
            P(),
            P("sp", "tp"),
            P("sp", "tp"),
            P("sp", "tp"),
            P(),
            P(),
            P("tp"),
            P("sp", "tp"),
            P("sp", "tp"),
            P("sp", "tp"),
            P(),
            P(),
            P("tp", "sp"),
            P("tp", "sp"),
        ),
        out_specs=P(("grp", "sp", "tp"), None),
        check_vma=False,
    )
```

```python
import functools

import jax
import jax.numpy as jnp
import numpy as np
from jax import lax
from jax.experimental import pallas as pl
from jax.experimental.pallas import tpu as pltpu
from jax.sharding import PartitionSpec as P

HD = 64
WINDOW = 128
GRID_W = 64


EPS = 1e-06
THETA = 10000.0


MESH = pl.DeviceIdType.MESH
HALVES = 2


class LineGather:
    def __init__(self, own, buf, z_recv, r_send, l_send, y_recv=None, y_send=None, axis=0):
        self.own, self.buf = own, buf
        self.z_recv, self.y_recv = z_recv, y_recv
        self.r_send, self.l_send, self.y_send = r_send, l_send, y_send
        self.n = lax.axis_size("sp")
        self.s = lax.axis_index("sp")
        self.shared = y_recv is not None
        self.g = lax.axis_index("grp") if self.shared else 0
        self.chunks = z_recv.shape[1]
        self.axis = axis
        extent = buf.shape[1 + axis]
        self.half = extent // HALVES if self.shared else extent
        self.size = self.half // self.chunks

    def rows(self, half, c):
        piece = pl.ds(pl.multiple_of(half * self.half + c * self.size, self.size), self.size)
        return (piece,) if self.axis == 0 else (slice(None), piece)

    def block(self, o, half, c):
        return self.buf.at[(o,) + self.rows(half, c)]

    def copy(self, src, o, c, sem, recv, target, half):
        return pltpu.make_async_remote_copy(
            src_ref=src,
            dst_ref=self.block(o, half, c),
            send_sem=sem.at[o, c],
            recv_sem=recv.at[o, c],
            device_id=target,
            device_id_type=MESH,
        )

    def right(self, src, o, c):
        return self.copy(src, o, c, self.r_send, self.z_recv, {"sp": lax.rem(self.s + 1, self.n)}, self.g)

    def left(self, src, o, c):
        return self.copy(
            src, o, c, self.l_send, self.z_recv, {"sp": lax.rem(self.s + self.n - 1, self.n)}, self.g
        )

    def twin(self, o, c, half):
        return self.copy(
            self.block(o, half, c), o, c, self.y_send, self.y_recv, {"grp": 1 - self.g}, half
        )

    def mine(self, c):
        if self.own is None:
            return self.block(self.s, self.g, c)
        return self.own.at[self.rows(self.g, c)]

    def start(self, first=0, last=None):
        for c in range(first, self.chunks if last is None else last):
            mine = self.mine(c)

            @pl.when(self.s + 1 < self.n)
            def _():
                self.right(mine, self.s, c).start()

            @pl.when(self.s > 0)
            def _():
                self.left(mine, self.s, c).start()

    def forward(self, d):
        for c in range(self.chunks):

            @pl.when(self.s - d >= 0)
            def _():
                o = self.s - d
                there = self.block(o, self.g, c)
                self.right(there, o, c).wait_recv()

                @pl.when(self.s + 1 < self.n)
                def _():
                    self.right(there, o, c).start()

                if self.shared:
                    self.twin(o, c, self.g).start()

            @pl.when(self.s + d < self.n)
            def _():
                o = self.s + d
                there = self.block(o, self.g, c)
                self.left(there, o, c).wait_recv()

                @pl.when(self.s > 0)
                def _():
                    self.left(there, o, c).start()

                if self.shared:
                    self.twin(o, c, self.g).start()

    def use(self, d, fn, near=None):
        for there, o in ((self.s - d >= 0, self.s - d), (self.s + d < self.n, self.s + d)):
            if near is not None:

                @pl.when(there)
                def _():
                    near(o)

        for there, o in ((self.s - d >= 0, self.s - d), (self.s + d < self.n, self.s + d)):

            @pl.when(there)
            def _():
                for c in range(self.chunks):
                    self.twin(o, c, 1 - self.g).wait_recv()
                fn(o)

    def run(self, fn, near=None, last=None):
        self.forward(1)
        self.rest(fn, near, last)

    def rest(self, fn, near=None, last=None):
        @pl.loop(2, self.n)
        def _(d):
            self.forward(d)
            self.use(d - 1, fn, near)

        if last is not None:
            last()
        self.use(self.n - 1, fn, near)

    def finish(self):
        @pl.loop(0, self.n)
        def _(o):
            for c in range(self.chunks):
                there = self.block(o, self.g, c)

                @pl.when((o <= self.s) & (self.s + 1 < self.n))
                def _():
                    self.right(there, o, c).wait_send()

                @pl.when((o >= self.s) & (self.s > 0))
                def _():
                    self.left(there, o, c).wait_send()

                if self.shared:

                    @pl.when(o != self.s)
                    def _():
                        self.twin(o, c, self.g).wait_send()


def greet():
    n, s, g = lax.axis_size("sp"), lax.axis_index("sp"), lax.axis_index("grp")
    n_tp, t = lax.axis_size("tp"), lax.axis_index("tp")
    barrier = pltpu.get_barrier_semaphore()
    pl.semaphore_signal(barrier, inc=1, device_id={"grp": 1 - g}, device_id_type=MESH)
    for j in range(1, n_tp):
        pl.semaphore_signal(barrier, inc=1, device_id={"tp": lax.rem(t + j, n_tp)}, device_id_type=MESH)

    @pl.when(s + 1 < n)
    def _():
        pl.semaphore_signal(barrier, inc=1, device_id={"sp": lax.rem(s + 1, n)}, device_id_type=MESH)

    @pl.when(s > 0)
    def _():
        pl.semaphore_signal(barrier, inc=1, device_id={"sp": lax.rem(s + n - 1, n)}, device_id_type=MESH)

    pl.semaphore_wait(barrier, n_tp + (s + 1 < n).astype(jnp.int32) + (s > 0).astype(jnp.int32))


LANES = 128


def by_half(low, high):
    lane = lax.broadcasted_iota(jnp.int32, low.shape, 1)
    return jnp.where(lane < HD, low, high)


def swap_pairs(values, reach):
    lane = lax.broadcasted_iota(jnp.int32, values.shape, 1)
    ahead = pltpu.roll(values, LANES - reach, 1)
    behind = pltpu.roll(values, reach, 1)
    return jnp.where(lax.rem(lane, 2 * reach) < reach, ahead, behind)


def head_tile(tile, kinds, gains_ref, tables_ref):
    square = tile * tile
    zero = jnp.zeros_like(square)
    low = jnp.sum(by_half(square, zero), axis=-1, keepdims=True)
    high = jnp.sum(by_half(zero, square), axis=-1, keepdims=True)
    mean = by_half(jnp.broadcast_to(low, tile.shape), jnp.broadcast_to(high, tile.shape)) * (1.0 / HD)
    scaled = tile * lax.rsqrt(mean + EPS)

    def one(kind):
        if kind is None:
            return tile
        gain, table, reach = kind
        normed = scaled * gains_ref[gain : gain + 1, :]
        return normed * tables_ref[2 * table] + swap_pairs(normed, reach) * tables_ref[2 * table + 1]

    if kinds[0] == kinds[1]:
        return one(kinds[0])
    return by_half(one(kinds[0]), one(kinds[1]))


def layer_kernel(
    sizes, x_ref, gain_ref, fixed_ref, g0, g1, g2, g3, sink_ref, *refs
):
    n_in = sizes[2]
    in_refs, out_refs = refs[:n_in], refs[n_in : n_in + 2]
    run_layer(sizes[:2], x_ref, gain_ref, fixed_ref, (g0, g1, g2, g3), sink_ref, in_refs, out_refs, *refs[n_in + 2 :])


def run_layer(
    sizes, x_ref, gain_ref, fixed_ref, head_gains, sink_ref, in_refs, out_refs, out_ref,
    small_ref, w_ref, wo_ref, tables_ref, load_sem, xn, proj, wbuf, wo_all, kvd, ext, qs, att, part, rs, halo_recv, halo_send, rs_recv, rs_send, *sems
):
    q_heads, kv_heads = sizes
    n, s = lax.axis_size("sp"), lax.axis_index("sp")
    n_tp, t = lax.axis_size("tp"), lax.axis_index("tp")
    depth = w_ref.shape[0]
    length = x_ref.shape[0]
    into = LineGather(w_ref, wbuf, *sems[:5])
    out = LineGather(wo_ref, wo_all, *sems[5:10], axis=1)
    keys = LineGather(None, kvd, *sems[10:])
    loads, at = [], 0
    for ref in in_refs:
        wide = ref.shape[1]
        loads.append(
            pltpu.make_async_copy(ref, w_ref.at[:, at : at + wide], load_sem.at[len(loads)])
        )
        at += wide
    at = 0
    for ref in out_refs:
        tall = ref.shape[0]
        loads.append(pltpu.make_async_copy(ref, wo_ref.at[at : at + tall], load_sem.at[len(loads)]))
        at += tall
    for load in loads:
        load.start()
    greet()
    for load in loads:
        load.wait()
    into.start()

    for k, ref in enumerate(head_gains):
        small_ref[k : k + 1, :] = jnp.concatenate([ref[...], ref[...]], axis=1)
    small_ref[4:8, :] = fixed_ref[...]
    step = 16

    @pl.loop(0, length // step)
    def _(i):
        rows = pl.ds(pl.multiple_of(i * step, step), step)
        values = x_ref[rows, :].astype(jnp.float32)
        mean = jnp.mean(values * values, axis=-1, keepdims=True)
        xn[rows, :] = (values * lax.rsqrt(mean + EPS) * gain_ref[...]).astype(jnp.bfloat16)

    def columns(o):
        return pl.ds(pl.multiple_of(o * depth, depth), depth)

    proj[...] = jnp.dot(xn[:, columns(s)], w_ref[...], preferred_element_type=jnp.float32)

    band = 64 if length % 64 == 0 else length

    @pl.loop(0, length // band)
    def _(i):
        rows = pl.ds(pl.multiple_of(i * band, band), band)
        shape = (band, LANES)
        place = lax.broadcasted_iota(jnp.int32, shape, 0) + (s * length + i * band)
        lane = lax.broadcasted_iota(jnp.int32, shape, 1)
        spot = jnp.where(lax.rem(lane, HD) < HD // 2, place // GRID_W, lax.rem(place, GRID_W))
        for k, where in enumerate((place, spot)):
            angles = where.astype(jnp.float32) * small_ref[4 + k : 5 + k, :]
            tables_ref[2 * k, rows, :] = jnp.cos(angles)
            tables_ref[2 * k + 1, rows, :] = jnp.sin(angles) * small_ref[6 + k : 7 + k, :]

    def add(o):
        proj[...] += jnp.dot(xn[:, columns(o)], wbuf[o], preferred_element_type=jnp.float32)

    into.run(add, last=lambda: out.start(0, 1))

    win_q, win_k, den_q, den_k = (0, 0, 32), (1, 0, 32), (2, 1, 16), (3, 1, 16)
    kinds = (
        [win_q] * q_heads + [den_q] * q_heads + [den_k] * kv_heads + [None] * kv_heads
        + [win_k] * kv_heads + [None] * kv_heads
    )
    q_tiles = 2 * q_heads * HD // LANES
    kv_tiles = 2 * kv_heads * HD // LANES

    def finished(i):
        return head_tile(
            proj[:, i * LANES : (i + 1) * LANES], kinds[2 * i : 2 * i + 2], small_ref, tables_ref
        )

    for i in range(kv_tiles):
        ext[WINDOW : WINDOW + length, i * LANES : (i + 1) * LANES] = finished(
            q_tiles + kv_tiles + i
        ).astype(jnp.bfloat16)
    for i in range(kv_tiles):
        kvd[s, :, i * LANES : (i + 1) * LANES] = finished(q_tiles + i).astype(jnp.bfloat16)

    def halo(side):
        source = pl.ds(length, WINDOW) if side == 0 else pl.ds(WINDOW, WINDOW)
        target = pl.ds(0, WINDOW) if side == 0 else pl.ds(WINDOW + length, WINDOW)
        peer = lax.rem(s + 1, n) if side == 0 else lax.rem(s + n - 1, n)
        return pltpu.make_async_remote_copy(
            src_ref=ext.at[source], dst_ref=ext.at[target], send_sem=halo_send.at[side],
            recv_sem=halo_recv.at[side], device_id={"sp": peer}, device_id_type=MESH,
        )

    has_right, has_left = s + 1 < n, s > 0

    @pl.when(has_right)
    def _():
        halo(0).start()

    @pl.when(has_left)
    def _():
        halo(1).start()

    keys.start()
    none = jnp.zeros((WINDOW, ext.shape[1]), jnp.bfloat16)

    @pl.when(jnp.logical_not(has_left))
    def _():
        ext[0:WINDOW, :] = none

    @pl.when(jnp.logical_not(has_right))
    def _():
        ext[WINDOW + length : WINDOW + length + WINDOW, :] = none

    group = q_heads // kv_heads

    def place(head):
        return head // 2, head % 2

    for i in range(q_tiles):
        tile = finished(i) * HD ** (-0.5)
        for b in range(2):
            head = 2 * i + b
            half = place((head % q_heads) // group)[1]
            moved = tile if half == b else pltpu.roll(tile, HD, 1)
            zero = jnp.zeros_like(moved)
            kept = by_half(moved, zero) if half == 0 else by_half(zero, moved)
            qs[head] = kept.astype(jnp.bfloat16)

    @pl.when(has_left)
    def _():
        halo(0).wait_recv()

    @pl.when(has_right)
    def _():
        halo(1).wait_recv()

    total_len = length * n

    def joined(results, heads):
        placed = []
        for b in range(2):
            half = place(kv_heads + heads[b] // group)[1]
            placed.append(results[b] if half == b else pltpu.roll(results[b], HD, 1))
        return by_half(placed[0], placed[1]).astype(jnp.bfloat16)

    def tile_of(head):
        return pl.ds(place(head)[0] * LANES, LANES)

    nt = (((1,), (1,)), ((), ()))

    def windowed(pair):
        @pl.loop(0, length // WINDOW)
        def _(b):
            base = pl.multiple_of(b * WINDOW, WINDOW)
            rows = pl.ds(base, WINDOW)
            near = pl.ds(base, 3 * WINDOW)
            shape = (WINDOW, 3 * WINDOW)
            at = lax.broadcasted_iota(jnp.int32, shape, 1) - WINDOW
            away = at - lax.broadcasted_iota(jnp.int32, shape, 0)
            pos = at + (s * length + base)
            valid = (away <= WINDOW) & (away >= -WINDOW) & (pos >= 0) & (pos < total_len)
            results = []
            for head in (2 * pair, 2 * pair + 1):
                key = ext[near, tile_of(head // group)]
                value = ext[near, tile_of(kv_heads + head // group)]
                scores = lax.dot_general(qs[head, rows, :], key, nt, preferred_element_type=jnp.float32)
                scores = jnp.where(valid, scores, -jnp.inf)
                floor = sink_ref[0, head]
                top = jnp.maximum(jnp.max(scores, axis=-1, keepdims=True), floor)
                expon = jnp.exp(scores - top)
                total = jnp.sum(expon, axis=-1, keepdims=True) + jnp.exp(floor - top)
                weights = (expon / total).astype(jnp.bfloat16)
                results.append(jnp.dot(weights, value, preferred_element_type=jnp.float32))
            att[rows, pair * LANES : (pair + 1) * LANES] = joined(results, (2 * pair, 2 * pair + 1))

    pairs = q_heads // 2
    keys.forward(1)
    windowed(0)

    @pl.loop(2, n)
    def _(d):
        keys.forward(d)

    out.start(1)
    for pair in range(1, pairs):
        windowed(pair)

    def dense(pair):
        @pl.loop(0, length // LANES)
        def _(b):
            rows = pl.ds(pl.multiple_of(b * LANES, LANES), LANES)
            results = []
            for head in (2 * pair, 2 * pair + 1):
                key = kvd[:, :, tile_of(head // group)].reshape(total_len, LANES)
                value = kvd[:, :, tile_of(kv_heads + head // group)].reshape(total_len, LANES)
                scores = lax.dot_general(
                    qs[q_heads + head, rows, :], key, nt, preferred_element_type=jnp.float32
                )
                top = jnp.max(scores, axis=-1, keepdims=True)
                expon = jnp.exp(scores - top)
                total = jnp.sum(expon, axis=-1, keepdims=True)
                summed = jnp.dot(
                    expon.astype(jnp.bfloat16), value, preferred_element_type=jnp.float32
                )
                results.append(summed / total)
            at = (pairs + pair) * LANES
            att[rows, at : at + LANES] = joined(results, (2 * pair, 2 * pair + 1))

    dense(0)
    out.forward(1)
    for pair in range(1, pairs):
        dense(pair)

    share = length // n_tp

    wide = wo_ref.shape[1]
    part_cols = wide // HALVES
    mine = lax.axis_index("grp")

    def span(h):
        return pl.ds(pl.multiple_of(h * part_cols, part_cols), part_cols)

    def exchange(o, h, j):
        peer = lax.rem(t + j, n_tp)
        return pltpu.make_async_remote_copy(
            src_ref=part.at[o, pl.ds(pl.multiple_of(peer * share, share), share), span(h)],
            dst_ref=rs.at[t, o, :, span(h)], send_sem=rs_send.at[j - 1, o, h],
            recv_sem=rs_recv.at[t, o, h], device_id={"tp": peer}, device_id_type=MESH,
        )

    def arrived(o, h, j):
        source = lax.rem(t + n_tp - j, n_tp)
        there = rs.at[source, o, :, span(h)]
        return pltpu.make_async_remote_copy(
            src_ref=there, dst_ref=there, send_sem=rs_send.at[j - 1, o, h],
            recv_sem=rs_recv.at[source, o, h], device_id={"tp": source}, device_id_type=MESH,
        )

    def emit(o, h, weight):
        part[o, :, span(h)] = jnp.dot(
            att[...], weight, preferred_element_type=jnp.float32
        ).astype(jnp.bfloat16)
        for j in range(1, n_tp):
            exchange(o, h, j).start()
        rs[t, o, :, span(h)] = part[o, pl.ds(pl.multiple_of(t * share, share), share), span(h)]

    def collect(o, h):
        for j in range(1, n_tp):
            arrived(o, h, j).wait_recv()
        total = rs[0, o, :, span(h)].astype(jnp.float32)
        for g in range(1, n_tp):
            total += rs[g, o, :, span(h)].astype(jnp.float32)
        columns_out = pl.ds(pl.multiple_of(o * wide + h * part_cols, part_cols), part_cols)
        out_ref[:, columns_out] = total.astype(jnp.bfloat16)

    for h in range(HALVES):
        emit(s, h, wo_ref[:, span(h)])
    out.rest(
        lambda o: emit(o, 1 - mine, wo_all[o, :, span(1 - mine)]),
        near=lambda o: emit(o, mine, wo_all[o, :, span(mine)]),
    )

    @pl.loop(0, n)
    def _(d):
        o = lax.rem(s + d, n)
        for h in range(HALVES):
            collect(o, h)

    @pl.loop(0, n)
    def _(o):
        for h in range(HALVES):
            for j in range(1, n_tp):
                exchange(o, h, j).wait_send()

    @pl.when(has_right)
    def _():
        halo(0).wait_send()

    @pl.when(has_left)
    def _():
        halo(1).wait_send()

    into.finish()
    out.finish()
    keys.finish()


def local(
    tokens_in,
    norm_gain,
    window_query,
    window_key,
    window_value,
    window_query_gain,
    window_key_gain,
    sink_logit,
    dense_query,
    dense_key,
    dense_value,
    dense_query_gain,
    dense_key_gain,
    window_out,
    dense_out,
):
    length, width = tokens_in.shape
    n, n_tp = lax.axis_size("sp"), lax.axis_size("tp")
    q_heads, kv_heads = window_query.shape[1] // HD, window_key.shape[1] // HD
    weights, held = [], []
    for weight in (window_query, dense_query, dense_key, dense_value, window_key, window_value):
        held.append(weight)
        if sum(w.shape[1] for w in held) % LANES == 0:
            weights.append(held[0] if len(held) == 1 else jnp.concatenate(held, axis=1))
            held = []
    depth, in_cols = window_query.shape[0], sum(w.shape[1] for w in weights)
    out_rows, out_cols = window_out.shape[0] + dense_out.shape[0], window_out.shape[1]

    lane = np.arange(LANES)
    fixed = np.stack(
        [THETA ** (-2.0 * (lane % (wide // 2)) / wide) for wide in (HD, HD // 2)]
        + [np.where(lane % wide < wide // 2, -1.0, 1.0) for wide in (HD, HD // 2)]
    ).astype(np.float32)
    gains = [g[None, :] for g in (window_query_gain, window_key_gain, dense_query_gain, dense_key_gain)]

    def gather(chunks):
        return [pltpu.SemaphoreType.DMA((n, chunks)) for _ in range(5)]

    in_chunks = 8 if n <= 4 else 1
    out_chunks = out_cols // HALVES // LANES if n <= 4 else 1
    kv_cols = 2 * kv_heads * HD
    vmem = pl.BlockSpec(memory_space=pltpu.VMEM)
    share = length // n_tp
    return pl.pallas_call(
        functools.partial(layer_kernel, (q_heads, kv_heads, len(weights))),
        out_shape=jax.ShapeDtypeStruct((share, width), jnp.bfloat16),
        in_specs=[vmem] * 7
        + [pl.BlockSpec(memory_space=pltpu.SMEM)]
        + [pl.BlockSpec(memory_space=pl.ANY)] * (len(weights) + 2),
        out_specs=vmem,
        scratch_shapes=[
            pltpu.VMEM((8, LANES), jnp.float32),
            pltpu.VMEM((depth, in_cols), jnp.bfloat16),
            pltpu.VMEM((out_rows, out_cols), jnp.bfloat16),
            pltpu.VMEM((4, length, LANES), jnp.float32),
            pltpu.SemaphoreType.DMA((len(weights) + 2,)),
            pltpu.VMEM((length, width), jnp.bfloat16),
            pltpu.VMEM((length, in_cols), jnp.float32),
            pltpu.VMEM((n, depth, in_cols), jnp.bfloat16),
            pltpu.VMEM((n, out_rows, out_cols), jnp.bfloat16),
            pltpu.VMEM((n, length, kv_cols), jnp.bfloat16),
            pltpu.VMEM((length + 2 * WINDOW, kv_cols), jnp.bfloat16),
            pltpu.VMEM((2 * q_heads, length, LANES), jnp.bfloat16),
            pltpu.VMEM((length, out_rows), jnp.bfloat16),
            pltpu.VMEM((n, length, out_cols), jnp.bfloat16),
            pltpu.VMEM((n_tp, n, share, out_cols), jnp.bfloat16),
            pltpu.SemaphoreType.DMA((2,)),
            pltpu.SemaphoreType.DMA((2,)),
            pltpu.SemaphoreType.DMA((n_tp, n, HALVES)),
            pltpu.SemaphoreType.DMA((n_tp - 1, n, HALVES)),
        ]
        + gather(in_chunks)
        + gather(out_chunks)
        + [pltpu.SemaphoreType.DMA((n, 2 if n <= 4 else 1)) for _ in range(3)],
        compiler_params=pltpu.CompilerParams(
            collective_id=0, has_side_effects=True, vmem_limit_bytes=62 * 1024 * 1024
        ),
    )(tokens_in, norm_gain[None, :], fixed, *gains, sink_logit[None, :], *weights, window_out, dense_out)


def solution(mesh):
    return jax.shard_map(
        local,
        mesh=mesh,
        in_specs=(
            P(("grp", "sp"), None),
            P(),
            P("sp", "tp"),
            P("sp", "tp"),
            P("sp", "tp"),
            P(),
            P(),
            P("tp"),
            P("sp", "tp"),
            P("sp", "tp"),
            P("sp", "tp"),
            P(),
            P(),
            P("tp", "sp"),
            P("tp", "sp"),
        ),
        out_specs=P(("grp", "sp", "tp"), None),
        check_vma=False,
    )
```
